32 devices in a mesh: grp: 2 (over y), kv: 4 (over z), tp: 4 (over x, core).
Axes of the slice: x: 2, y: 2, z: 4, core: 2. Of those that a mesh axis runs over, the one named last changes fastest.
Arguments:
- stream_in: bfloat16 [96, 4096], P(('grp', 'tp'), 'kv'), parts along dimension 0, may hold values from -40 to 40
- positions: int32 [96], P(('grp', 'kv')), parts along dimension 0, may hold values from 1024 to 32767
- ret_state: float32 [96, 16, 128, 128], P(('grp', 'kv'), 'tp'), parts along dimension 0, may hold values from -0.6 to 0.6
- first_gain: float32 [4096], P('kv'), may hold values from 0.1 to 1.9
- first_gate: bfloat16 [4096, 11008], P('kv', 'tp'), may hold values from -0.09375 to 0.09375
- first_up: bfloat16 [4096, 11008], P('kv', 'tp'), may hold values from -0.09375 to 0.09375
- first_down: bfloat16 [11008, 4096], P('tp', 'kv'), may hold values from -0.1875 to 0.1875
- mix_gain: float32 [4096], P('kv'), may hold values from 0.1 to 1.9
- w_query: bfloat16 [4096, 2048], P('kv', 'tp'), may hold values from -0.09375 to 0.09375
- w_key: bfloat16 [4096, 2048], P('kv', 'tp'), may hold values from -0.09375 to 0.09375
- w_value: bfloat16 [4096, 2048], P('kv', 'tp'), may hold values from -0.09375 to 0.09375
- w_outgate: bfloat16 [4096, 2048], P('kv', 'tp'), may hold values from -0.09375 to 0.09375
- w_out: bfloat16 [2048, 4096], P('tp', 'kv'), may hold values from -0.21875 to 0.21875
- head_gain: float32 [2048], P('tp'), may hold values from 0.1 to 1.9
- second_gain: float32 [4096], P('kv'), may hold values from 0.1 to 1.9
- second_gate: bfloat16 [4096, 11008], P('kv', 'tp'), may hold values from -0.09375 to 0.09375
- second_up: bfloat16 [4096, 11008], P('kv', 'tp'), may hold values from -0.09375 to 0.09375
- second_down: bfloat16 [11008, 4096], P('tp', 'kv'), may hold values from -0.1875 to 0.1875
Outputs:
- stream_out: bfloat16 [96, 4096], P(('grp', 'tp'), 'kv'), parts along dimension 0
- new_state: float32 [96, 16, 128, 128], P(('grp', 'kv'), 'tp'), parts along dimension 0
The draws below stay inside these ranges and needn't reach their ends.
There are 2 independent parts, one for each index of `grp`. The reference program is written for one: setup_inputs(seed, part) draws one part's arguments, and reference() takes and returns one part's arrays. A program takes and returns all parts, laid end to end along the dimension named above; an argument that names none is the same for every part. Nothing has to cross between parts.
All inputs are finite; a program needn't handle non-finite values.
Results may differ from the reference program's by a relative error of at most 0.03.
Values may be sent and summed in bfloat16 or wider, within the bound.
A program may use at most 128 MiB of HBM per device.

```python
import jax
import jax.numpy as jnp
from jax import lax

D = 4096
FF = 11008
HEADS = 16
HEAD_DIM = 128
BATCH = 48
RET_WIDTH = 2048


def draw_stream_in(key, part):
    base_key, column_key, row_key = jax.random.split(jax.random.fold_in(key, 17), 3)
    columns = jnp.arange(D, dtype=jnp.float32) / D
    base = jax.random.truncated_normal(base_key, -4.0, 4.0, (BATCH, D), jnp.float32)
    column_scale = jnp.exp(0.5 * jnp.log(10.0) * (columns + jax.random.uniform(column_key, (D,), jnp.float32)))
    row_scale = jnp.exp(jax.random.uniform(row_key, (BATCH, 1), jnp.float32, 0.0, jnp.log(3.0)))
    return (0.3 * base * column_scale[None, :] * row_scale).astype(jnp.bfloat16)


def place_ends(result, stream_key, least, largest):
    place = [jax.random.randint(jax.random.fold_in(stream_key, axis), (), 0, length) for axis, length in enumerate(result.shape)]
    widest = result.shape.index(max(result.shape))
    neighbour = place[:widest] + [(place[widest] + 1) % result.shape[widest]] + place[widest + 1:]
    return result.at[tuple(place)].set(least).at[tuple(neighbour)].set(largest)


def block_levels(key, dims, cuts, low, high):
    loudness, own = 1.0, jax.random.fold_in(key, 6)
    for position, shards_of in cuts:
        draws = jnp.exp(jax.random.uniform(jax.random.fold_in(own, position), (shards_of,), jnp.float32, low / len(cuts), high / len(cuts)))
        loudness = loudness * jnp.repeat(draws, dims[position] // shards_of).reshape([-1 if axis == position else 1 for axis in range(len(dims))])
    return loudness


def bell_draw(rng, dims, width, limit, cuts=(), kind=jnp.bfloat16):
    loudness = block_levels(rng, dims, cuts, -0.22, 0.18) if cuts else 1.0
    values = jax.random.normal(rng, dims, jnp.float32) * width * loudness
    return jnp.minimum(jnp.maximum(values, -limit), limit).astype(kind)


def setup_inputs(seed: int = 0, part: int = 0) -> dict:
    keys = jax.random.split(jax.random.key(seed), 19)
    part_splits = jax.random.split(jax.random.fold_in(keys[18], part), 19)
    stream_in = draw_stream_in(jax.random.fold_in(jax.random.fold_in(keys[18], part), 71), part)
    positions = place_ends(jax.random.randint(part_splits[1], (BATCH,), 1024, 32768), jax.random.fold_in(part_splits[1], 1), 1024, 32767).astype(jnp.int32)
    ret_state = bell_draw(part_splits[2], (BATCH, HEADS, HEAD_DIM, HEAD_DIM), 0.1, 0.6, ((0, 4), (1, 4)), jnp.float32)
    first_gain = jnp.clip(1.0 + 0.18 * jax.random.normal(keys[3], (D,), jnp.float32), 0.1, 1.9)
    first_gate = bell_draw(keys[4], (D, FF), D ** -0.5, 0.09375, ((0, 4), (1, 4)))
    first_up = bell_draw(keys[5], (D, FF), D ** -0.5, 0.09375, ((0, 4), (1, 4)))
    first_down = bell_draw(keys[6], (FF, D), (FF // 12) ** -0.5, 0.1875, ((0, 4), (1, 4)))
    mix_gain = jnp.clip(1.0 + 0.18 * jax.random.normal(keys[7], (D,), jnp.float32), 0.1, 1.9)
    w_query = bell_draw(keys[8], (D, RET_WIDTH), D ** -0.5, 0.09375, ((0, 4), (1, 4)))
    w_key = bell_draw(keys[9], (D, RET_WIDTH), D ** -0.5, 0.09375, ((0, 4), (1, 4)))
    w_value = bell_draw(keys[10], (D, RET_WIDTH), D ** -0.5, 0.09375, ((0, 4), (1, 4)))
    w_outgate = bell_draw(keys[11], (D, RET_WIDTH), D ** -0.5, 0.09375, ((0, 4), (1, 4)))
    w_out = bell_draw(keys[12], (RET_WIDTH, D), (RET_WIDTH // 3) ** -0.5, 0.21875, ((0, 4), (1, 4)))
    head_gain = jnp.clip(1.0 + 0.18 * jax.random.normal(keys[13], (RET_WIDTH,), jnp.float32), 0.1, 1.9)
    second_gain = jnp.clip(1.0 + 0.18 * jax.random.normal(keys[14], (D,), jnp.float32), 0.1, 1.9)
    second_gate = bell_draw(keys[15], (D, FF), D ** -0.5, 0.09375, ((0, 4), (1, 4)))
    second_up = bell_draw(keys[16], (D, FF), D ** -0.5, 0.09375, ((0, 4), (1, 4)))
    second_down = bell_draw(keys[17], (FF, D), (FF // 12) ** -0.5, 0.1875, ((0, 4), (1, 4)))
    return {"stream_in": stream_in, "positions": positions, "ret_state": ret_state, "first_gain": first_gain, "first_gate": first_gate, "first_up": first_up, "first_down": first_down, "mix_gain": mix_gain, "w_query": w_query, "w_key": w_key, "w_value": w_value, "w_outgate": w_outgate, "w_out": w_out, "head_gain": head_gain, "second_gain": second_gain, "second_gate": second_gate, "second_up": second_up, "second_down": second_down}


EPS_NORM = 1e-06
EPS_GROUP = 1e-05

def prepare(stream, norm_gain):
    widened = stream.astype(jnp.float32)
    squares = lax.optimization_barrier(jnp.sum(widened * widened, axis=1))
    scaled = (widened * norm_gain.astype(jnp.float32)).astype(jnp.bfloat16)
    factor = lax.rsqrt(squares / D + EPS_NORM)[:, None]
    return (factor, scaled)

def feed_forward(stream, norm_gain, w_gate, w_up, w_down):
    factor, scaled = prepare(stream, norm_gain)
    gate_pre = factor * jnp.dot(scaled, w_gate, preferred_element_type=jnp.float32)
    up_pre = factor * jnp.dot(scaled, w_up, preferred_element_type=jnp.float32)
    hidden = (jax.nn.silu(gate_pre) * up_pre).astype(jnp.bfloat16)
    return (stream.astype(jnp.float32) + 0.5 * jnp.dot(hidden, w_down, preferred_element_type=jnp.float32)).astype(jnp.bfloat16)

def rotate(values_in, cosine, sine_part):
    half_dim = values_in.shape[-1] // 2
    lower_half = values_in[..., :half_dim]
    upper_half = values_in[..., half_dim:]
    return jnp.concatenate([lower_half * cosine - upper_half * sine_part, lower_half * sine_part + upper_half * cosine], axis=-1)

def reference(stream_in, positions, ret_state, first_gain, first_gate, first_up, first_down, mix_gain, w_query, w_key, w_value, w_outgate, w_out, head_gain, second_gain, second_gate, second_up, second_down):
    stream = feed_forward(stream_in, first_gain, first_gate, first_up, first_down)
    factor, scaled = prepare(stream, mix_gain)
    shape_heads = (BATCH, HEADS, HEAD_DIM)
    queries = (factor * jnp.dot(scaled, w_query, preferred_element_type=jnp.float32)).reshape(shape_heads)
    key_vec = (factor * jnp.dot(scaled, w_key, preferred_element_type=jnp.float32)).reshape(shape_heads)
    values_new = (factor * jnp.dot(scaled, w_value, preferred_element_type=jnp.float32)).reshape(shape_heads)
    gate_pre = (factor * jnp.dot(scaled, w_outgate, preferred_element_type=jnp.float32)).reshape(shape_heads)
    half_dim = HEAD_DIM // 2
    inverse = 10000.0 ** (-jnp.arange(half_dim, dtype=jnp.float32) / half_dim)
    angles = positions.astype(jnp.float32)[:, None] * inverse[None, :]
    cosine = jnp.cos(angles)[:, None, :]
    sine_part = jnp.sin(angles)[:, None, :]
    queries = rotate(queries, cosine, sine_part)
    key_vec = rotate(key_vec, cosine, sine_part) * HEAD_DIM ** (-0.5)
    head_ids = jnp.arange(HEADS).astype(jnp.float32)
    decays = jnp.exp(jnp.log1p(-2.0 ** (-5.0 - head_ids)))
    carried = jnp.einsum('shd,shde->she', queries, ret_state, precision=lax.Precision.HIGHEST)
    within = lax.optimization_barrier(jnp.sum(queries * key_vec, axis=-1, keepdims=True))
    mixture = decays[None, :, None] * carried + within * values_new
    new_state = decays[None, :, None, None] * ret_state + key_vec[..., :, None] * values_new[..., None, :]
    average = lax.optimization_barrier(jnp.mean(mixture, axis=-1, keepdims=True))
    centered = mixture - average
    variance = lax.optimization_barrier(jnp.mean(centered * centered, axis=-1, keepdims=True))
    normed = centered * lax.rsqrt(variance + EPS_GROUP) * head_gain.astype(jnp.float32).reshape(HEADS, HEAD_DIM)
    ret_out = (jax.nn.silu(gate_pre) * normed).astype(jnp.bfloat16).reshape(BATCH, RET_WIDTH)
    stream = (stream.astype(jnp.float32) + jnp.dot(ret_out, w_out, preferred_element_type=jnp.float32)).astype(jnp.bfloat16)
    stream = feed_forward(stream, second_gain, second_gate, second_up, second_down)
    return (stream, new_state)
```

```python
import functools

import jax
import jax.numpy as jnp
import numpy as np
from jax import lax
from jax.experimental import pallas as pl
from jax.experimental.pallas import tpu as pltpu
from jax.sharding import PartitionSpec as P

MESH = pl.DeviceIdType.MESH
EPS_NORM = 1e-06
EPS_GROUP = 1e-05
PIECE = 256
F32 = jnp.float32
BF16 = jnp.bfloat16


def silu(v):
    return v / (1.0 + jnp.exp(-v))


def layer_kernel(
    kv, tp, share,
    stream_ref, cos_ref, sin_ref, gain1_ref, gain_mix_ref, gain2_ref, head_gain_ref,
    gate1_hbm, up1_hbm, down1_hbm, wq_hbm, wk_hbm, wv_hbm, wg_hbm, wo_hbm,
    gate2_hbm, up2_hbm, down2_hbm, state_hbm,
    out_ref, key_out_ref, value_out_ref,
    gate1, up1, down1, wq, wk, wv, wg, wo, gate2, up2, down2, state,
    stream_slots, part_send, part_recv, wide, lhs, acc, sq_slots, inverse,
    ff_send, ff_recv, hidden, proj, proj_send, proj_recv, row_sq, row_sq_send, row_sq_recv,
    padded, carried, ret_slots, mixed,
    load_sem, tp_send_sem, tp_recv_sem, sq_send_sem, sq_recv_sem,
    ff_send_sem, ff_recv_sem, hid_send_sem, hid_recv_sem,
    proj_send_sem, proj_recv_sem, row_send_sem, row_recv_sem, ret_send_sem, ret_recv_sem,
):
    me_k = lax.axis_index("kv")
    me_t = lax.axis_index("tp")
    rows, width = wide.shape
    model = width * kv
    units = gate1.shape[1]
    pieces = -(-units // PIECE)
    ragged = units - (pieces - 1) * PIECE
    rows_t = rows // tp
    rows_k = rows // kv
    half = max(1, kv // 2)
    heads = state.shape[1]
    hd = state.shape[2]
    qw = heads * hd

    loads = []
    order = [
        (gate1_hbm, gate1), (up1_hbm, up1), (down1_hbm, down1), (wq_hbm, wq), (wk_hbm, wk),
        (wv_hbm, wv), (wg_hbm, wg), (state_hbm, state), (wo_hbm, wo),
        (gate2_hbm, gate2), (up2_hbm, up2), (down2_hbm, down2),
    ]
    for n, (src, dst) in enumerate(order):
        copy = pltpu.make_async_copy(src, dst, load_sem.at[n])
        copy.start()
        loads.append(copy)

    barrier = pltpu.get_barrier_semaphore()
    for j in range(1, kv):
        pl.semaphore_signal(barrier, 1, device_id={"kv": lax.rem(me_k + j, kv)}, device_id_type=MESH)
    for j in range(1, tp):
        pl.semaphore_signal(barrier, 1, device_id={"tp": lax.rem(me_t + j, tp)}, device_id_type=MESH)
    pl.semaphore_wait(barrier, kv + tp - 2)

    pending = []

    def exchange(axis, me, n, src_of, dst, send_sem, recv_sem):
        for j in range(1, n):
            dest = lax.rem(me + j, n)
            copy = pltpu.make_async_remote_copy(
                src_ref=src_of(dest), dst_ref=dst.at[me],
                send_sem=send_sem.at[dest], recv_sem=recv_sem.at[me],
                device_id={axis: dest}, device_id_type=MESH,
            )
            copy.start()
            pending.append(copy)

        def arrive():
            for j in range(1, n):
                source = lax.rem(me + j, n)
                pltpu.make_async_remote_copy(
                    src_ref=dst.at[source], dst_ref=dst.at[source],
                    send_sem=send_sem.at[source], recv_sem=recv_sem.at[source],
                    device_id={axis: source}, device_id_type=MESH,
                ).wait_recv()

        return arrive

    def gather_stream(phase):
        slots = stream_slots.at[phase]
        return exchange(
            "tp", me_t, tp, lambda dest: slots.at[me_t], slots,
            tp_send_sem.at[phase], tp_recv_sem.at[phase],
        )

    def widen(phase, arrive, gain_ref):
        arrive()
        for t in range(tp):
            wide[t * rows_t : (t + 1) * rows_t, :] = stream_slots[phase, t].astype(F32)
        stream = wide[...]
        lhs[...] = (stream * gain_ref[...]).astype(BF16)
        return jnp.sum(stream * stream, axis=1, keepdims=True)

    def order_of(k):
        side = lax.rem(me_k // half + 1 + k // half, 2) if kv > 1 else 0
        return side * half + lax.rem(lax.rem(me_k, half) + 1 + lax.rem(k, half), half)

    def advance(phase, factor, last):
        for t in range(tp):
            part_send[phase, t] = acc[t * rows_t : (t + 1) * rows_t, :].astype(BF16)
        slots = part_recv.at[phase]
        arrive = exchange(
            "tp", me_t, tp, lambda dest: part_send.at[phase, dest], slots,
            tp_send_sem.at[3 + phase], tp_recv_sem.at[3 + phase],
        )
        total = part_send[phase, me_t].astype(F32)
        arrive()
        for j in range(1, tp):
            total = total + part_recv[phase, lax.rem(me_t + j, tp)].astype(F32)
        fresh = (stream_slots[phase, me_t].astype(F32) + factor * total).astype(BF16)
        if last:
            out_ref[...] = fresh
            return None
        stream_slots[phase + 1, me_t] = fresh
        return gather_stream(phase + 1)

    def feed_forward(block, phase, arrive, gain_ref, w_gate, w_up, w_down, waits):
        squares = widen(phase, arrive, gain_ref)
        sq_slots[block, me_k] = jnp.broadcast_to(squares, (rows, 128))
        sq = sq_slots.at[block]
        sq_arrive = exchange(
            "kv", me_k, kv, lambda dest: sq.at[me_k], sq, sq_send_sem.at[block], sq_recv_sem.at[block]
        )
        waits[0].wait()
        waits[1].wait()

        def piece_copy(dest, p):
            return pltpu.make_async_remote_copy(
                src_ref=ff_send.at[block, dest, p], dst_ref=ff_recv.at[block, me_k, p],
                send_sem=ff_send_sem.at[block, dest, p], recv_sem=ff_recv_sem.at[block, me_k, p],
                device_id={"kv": dest}, device_id_type=MESH,
            )

        def on_piece(i, _):
            dest = order_of(i // share)
            p = lax.rem(i, share)
            g = dest * share + p

            def multiply(columns, n):
                left = lhs[...]
                for which, w in enumerate((w_gate, w_up)):
                    ff_send[block, dest, p, which, :, 0:n] = jnp.dot(
                        left, w[:, columns], preferred_element_type=F32
                    ).astype(BF16)

            @pl.when(g < pieces - 1)
            def _():
                multiply(pl.ds(pl.multiple_of(g * PIECE, PIECE), PIECE), PIECE)

            @pl.when(g == pieces - 1)
            def _():
                if ragged < PIECE:
                    for which in range(2):
                        ff_send[block, dest, p, which] = jnp.zeros((rows, PIECE), BF16)
                multiply(slice((pieces - 1) * PIECE, units), ragged)

            @pl.when((g < pieces) & (dest != me_k))
            def _():
                piece_copy(dest, p).start()

            return 0

        lax.fori_loop(0, kv * share, on_piece, 0)
        sq_arrive()
        total = sq_slots[block, 0]
        for k in range(1, kv):
            total = total + sq_slots[block, k]
        inverse[...] = lax.rsqrt(total / model + EPS_NORM)

        def hidden_copy(dest, p):
            slot = hidden.at[block, me_k * share + p]
            return pltpu.make_async_remote_copy(
                src_ref=slot, dst_ref=slot,
                send_sem=hid_send_sem.at[block, dest, p], recv_sem=hid_recv_sem.at[block, me_k, p],
                device_id={"kv": dest}, device_id_type=MESH,
            )

        def on_shard(p, _):
            @pl.when(me_k * share + p < pieces)
            def _():
                for j in range(1, kv):
                    source = lax.rem(me_k + j, kv)
                    slot = ff_recv.at[block, source, p]
                    pltpu.make_async_remote_copy(
                        src_ref=slot, dst_ref=slot,
                        send_sem=ff_send_sem.at[block, source, p],
                        recv_sem=ff_recv_sem.at[block, source, p],
                        device_id={"kv": source}, device_id_type=MESH,
                    ).wait_recv()
                sums = []
                for which in range(2):
                    total = ff_send[block, me_k, p, which].astype(F32)
                    for j in range(1, kv):
                        total = total + ff_recv[block, lax.rem(me_k + j, kv), p, which].astype(F32)
                    sums.append(total * inverse[:, 0:1])
                hidden[block, me_k * share + p] = (silu(sums[0]) * sums[1]).astype(BF16)
                for j in range(1, kv):
                    hidden_copy(order_of(j - 1), p).start()

            return 0

        lax.fori_loop(0, share, on_shard, 0)
        acc[...] = jnp.zeros_like(acc)
        waits[2].wait()

        def on_hidden(i, _):
            source = order_of(kv - 1 - i // share)
            p = lax.rem(i, share)
            g = source * share + p

            @pl.when((g < pieces) & (source != me_k))
            def _():
                slot = hidden.at[block, g]
                pltpu.make_async_remote_copy(
                    src_ref=slot, dst_ref=slot,
                    send_sem=hid_send_sem.at[block, source, p],
                    recv_sem=hid_recv_sem.at[block, source, p],
                    device_id={"kv": source}, device_id_type=MESH,
                ).wait_recv()

            @pl.when(g < pieces - 1)
            def _():
                depth = pl.ds(pl.multiple_of(g * PIECE, PIECE), PIECE)
                acc[...] += jnp.dot(hidden[block, g], w_down[depth, :], preferred_element_type=F32)

            @pl.when(g == pieces - 1)
            def _():
                acc[...] += jnp.dot(
                    hidden[block, pieces - 1, :, 0:ragged],
                    w_down[(pieces - 1) * PIECE : units, :],
                    preferred_element_type=F32,
                )

            return 0

        lax.fori_loop(0, kv * share, on_hidden, 0)

        def finish():
            def on_sent(i, _):
                dest = order_of(i // share)
                p = lax.rem(i, share)

                @pl.when((dest * share + p < pieces) & (dest != me_k))
                def _():
                    piece_copy(dest, p).wait_send()

                @pl.when((me_k * share + p < pieces) & (dest != me_k))
                def _():
                    hidden_copy(dest, p).wait_send()

                return 0

            lax.fori_loop(0, kv * share, on_sent, 0)

        return finish

    stream_slots[0, me_t] = stream_ref[...]
    arrive = gather_stream(0)
    finish1 = feed_forward(0, 0, arrive, gain1_ref, gate1, up1, down1, loads[0:3])
    arrive = advance(0, 0.5, False)

    squares = widen(1, arrive, gain_mix_ref)
    row_sq[...] = jnp.broadcast_to(squares, (rows, 128))
    for k in range(kv):
        row_sq_send[k] = row_sq[k * rows_k : (k + 1) * rows_k, :]
    row_arrive = exchange(
        "kv", me_k, kv, lambda dest: row_sq_send.at[dest], row_sq_recv, row_send_sem, row_recv_sem
    )
    arrivals = []
    for n, w in enumerate((wq, wk, wv, wg)):
        loads[3 + n].wait()
        proj[...] = jnp.dot(lhs[...], w[...], preferred_element_type=F32)
        for k in range(kv):
            proj_send[n, k] = proj[k * rows_k : (k + 1) * rows_k, :].astype(BF16)
        arrivals.append(
            exchange(
                "kv", me_k, kv, lambda dest, n=n: proj_send.at[n, dest], proj_recv.at[n],
                proj_send_sem.at[n], proj_recv_sem.at[n],
            )
        )
    loads[7].wait()
    row_arrive()
    total = row_sq_send[me_k]
    for j in range(1, kv):
        total = total + row_sq_recv[lax.rem(me_k + j, kv)]
    factor = lax.rsqrt(total / model + EPS_NORM)[:, 0:1]

    def projected(n):
        arrivals[n]()
        value = proj_send[n, me_k].astype(F32)
        for j in range(1, kv):
            value = value + proj_recv[n, lax.rem(me_k + j, kv)].astype(F32)
        return value * factor

    cosine, sine = cos_ref[...], sin_ref[...]

    def rotated(value, scale):
        parts = []
        for h in range(heads):
            x = value[:, h * hd : (h + 1) * hd]
            parts.append((x * cosine + pltpu.roll(x, hd // 2, 1) * sine) * scale)
        return parts

    queries = rotated(projected(0), 1.0)
    keys = rotated(projected(1), hd ** (-0.5))
    for h in range(heads):
        padded[h, 0:rows_k, :] = queries[h]
        key_out_ref[:, h * hd : (h + 1) * hd] = keys[h]
    for h in range(heads):
        turned = padded[h].T
        for s in range(rows_k):
            carried[h, s : s + 1, :] = jnp.sum(turned[:, s : s + 1] * state[s, h], axis=0, keepdims=True)
    values = projected(2)
    value_out_ref[...] = values
    gates = silu(projected(3))
    for h in range(heads):
        head = slice(h * hd, (h + 1) * hd)
        exponent = jnp.full((1, hd), me_t * heads + h, jnp.int32).astype(F32)
        decay = 1.0 - jnp.exp2(-5.0 - exponent)
        within = jnp.sum(queries[h] * keys[h], axis=1, keepdims=True)
        mixture = decay * carried[h, 0:rows_k, :] + within * values[:, head]
        centered = mixture - jnp.mean(mixture, axis=1, keepdims=True)
        variance = jnp.mean(centered * centered, axis=1, keepdims=True)
        normed = centered * lax.rsqrt(variance + EPS_GROUP) * head_gain_ref[:, head]
        ret_slots[me_k, :, head] = (gates[:, head] * normed).astype(BF16)
    ret_arrive = exchange(
        "kv", me_k, kv, lambda dest: ret_slots.at[me_k], ret_slots, ret_send_sem, ret_recv_sem
    )
    loads[8].wait()
    ret_arrive()
    for k in range(kv):
        mixed[k * rows_k : (k + 1) * rows_k, :] = ret_slots[k].astype(F32)
    acc[...] = jnp.dot(mixed[...].astype(BF16), wo[...], preferred_element_type=F32)
    arrive = advance(1, 1.0, False)
    finish2 = feed_forward(1, 2, arrive, gain2_ref, gate2, up2, down2, loads[9:12])
    advance(2, 0.5, True)
    finish1()
    finish2()
    for copy in pending:
        copy.wait_send()


def solution(mesh):
    kv, tp = mesh.shape["kv"], mesh.shape["tp"]

    def per_device(
        stream_in, positions, ret_state, first_gain, first_gate, first_up, first_down, mix_gain,
        w_query, w_key, w_value, w_outgate, w_out, head_gain, second_gain, second_gate, second_up,
        second_down,
    ):
        rows_t, width = stream_in.shape
        rows = rows_t * tp
        seqs, heads, hd, _ = ret_state.shape
        qw = heads * hd
        units = first_gate.shape[1]
        share = -(-(-(-units // PIECE)) // kv)
        half_dim = hd // 2
        freq = 10000.0 ** (-jnp.arange(half_dim, dtype=F32) / half_dim)
        angles = positions.astype(F32)[:, None] * freq[None, :]
        cosine, sine = jnp.cos(angles), jnp.sin(angles)
        cosine = jnp.concatenate([cosine, cosine], axis=1)
        sine = jnp.concatenate([-sine, sine], axis=1)
        weights = (
            first_gate, first_up, first_down, w_query, w_key, w_value, w_outgate, w_out,
            second_gate, second_up, second_down,
        )
        vmem = pl.BlockSpec(memory_space=pltpu.VMEM)
        anywhere = pl.BlockSpec(memory_space=pl.ANY)
        dma = pltpu.SemaphoreType.DMA
        pad_rows = -(-seqs // 16) * 16
        out, keys, values = pl.pallas_call(
            functools.partial(layer_kernel, kv, tp, share),
            out_shape=(
                jax.ShapeDtypeStruct((rows_t, width), BF16),
                jax.ShapeDtypeStruct((seqs, qw), F32),
                jax.ShapeDtypeStruct((seqs, qw), F32),
            ),
            in_specs=[vmem] * 7 + [anywhere] * 12,
            out_specs=(vmem, vmem, vmem),
            scratch_shapes=[pltpu.VMEM(w.shape, BF16) for w in weights]
            + [
                pltpu.VMEM(ret_state.shape, F32),
                pltpu.VMEM((3, tp, rows_t, width), BF16),
                pltpu.VMEM((3, tp, rows_t, width), BF16),
                pltpu.VMEM((3, tp, rows_t, width), BF16),
                pltpu.VMEM((rows, width), F32),
                pltpu.VMEM((rows, width), BF16),
                pltpu.VMEM((rows, width), F32),
                pltpu.VMEM((2, kv, rows, 128), F32),
                pltpu.VMEM((rows, 128), F32),
                pltpu.VMEM((2, kv, share, 2, rows, PIECE), BF16),
                pltpu.VMEM((2, kv, share, 2, rows, PIECE), BF16),
                pltpu.VMEM((2, kv * share, rows, PIECE), BF16),
                pltpu.VMEM((rows, qw), F32),
                pltpu.VMEM((4, kv, seqs, qw), BF16),
                pltpu.VMEM((4, kv, seqs, qw), BF16),
                pltpu.VMEM((rows, 128), F32),
                pltpu.VMEM((kv, seqs, 128), F32),
                pltpu.VMEM((kv, seqs, 128), F32),
                pltpu.VMEM((heads, pad_rows, hd), F32),
                pltpu.VMEM((heads, pad_rows, hd), F32),
                pltpu.VMEM((kv, seqs, qw), BF16),
                pltpu.VMEM((rows, qw), F32),
                dma((12,)), dma((6, tp)), dma((6, tp)), dma((2, kv)), dma((2, kv)),
                dma((2, kv, share)), dma((2, kv, share)), dma((2, kv, share)), dma((2, kv, share)),
                dma((4, kv)), dma((4, kv)), dma((kv,)), dma((kv,)), dma((kv,)), dma((kv,)),
            ],
            compiler_params=pltpu.CompilerParams(
                collective_id=0, has_side_effects=True, vmem_limit_bytes=63 * 1024 * 1024
            ),
        )(
            stream_in, cosine, sine, first_gain[None, :], mix_gain[None, :], second_gain[None, :],
            head_gain[None, :], *weights[0:8], *weights[8:11], ret_state,
        )
        head_ids = (lax.axis_index("tp") * heads + jnp.arange(heads)).astype(F32)
        decays = 1.0 - 2.0 ** (-5.0 - head_ids)
        keys = keys.reshape(seqs, heads, hd)
        values = values.reshape(seqs, heads, hd)
        new_state = (
            decays[None, :, None, None] * ret_state + keys[..., :, None] * values[..., None, :]
        )
        return out, new_state

    in_specs = (
        P(("grp", "tp"), "kv"), P(("grp", "kv")), P(("grp", "kv"), "tp", None, None), P("kv"),
        P("kv", "tp"), P("kv", "tp"), P("tp", "kv"), P("kv"), P("kv", "tp"), P("kv", "tp"),
        P("kv", "tp"), P("kv", "tp"), P("tp", "kv"), P("tp"), P("kv"), P("kv", "tp"),
        P("kv", "tp"), P("tp", "kv"),
    )
    out_specs = (P(("grp", "tp"), "kv"), P(("grp", "kv"), "tp", None, None))
    return jax.shard_map(
        per_device, mesh=mesh, in_specs=in_specs, out_specs=out_specs, check_vma=False
    )
```

```python
import functools

import jax
import jax.numpy as jnp
import numpy as np
from jax import lax
from jax.experimental import pallas as pl
from jax.experimental.pallas import tpu as pltpu
from jax.sharding import PartitionSpec as P

MESH = pl.DeviceIdType.MESH
EPS_NORM = 1e-06
EPS_GROUP = 1e-05
PIECE = 256
F32 = jnp.float32
BF16 = jnp.bfloat16


def silu(v):
    return v / (1.0 + jnp.exp(-v))


def layer_kernel(
    kv, tp, share,
    stream_ref, cos_ref, sin_ref, gain1_ref, gain_mix_ref, gain2_ref, head_gain_ref,
    gate1_hbm, up1_hbm, down1_hbm, wq_hbm, wk_hbm, wv_hbm, wg_hbm, wo_hbm,
    gate2_hbm, up2_hbm, down2_hbm, state_hbm,
    out_ref, key_out_ref, value_out_ref,
    gate1, up1, down1, wq, wk, wv, wg, wo, gate2, up2, down2, state,
    stream_slots, part_send, part_recv, wide, lhs, acc, sq_slots, inverse,
    ff_send, ff_recv, hidden, proj, proj_send, proj_recv, row_sq, row_sq_send, row_sq_recv,
    padded, carried, ret_slots, mixed,
    load_sem, tp_send_sem, tp_recv_sem, sq_send_sem, sq_recv_sem,
    ff_send_sem, ff_recv_sem, hid_send_sem, hid_recv_sem,
    proj_send_sem, proj_recv_sem, row_send_sem, row_recv_sem, ret_send_sem, ret_recv_sem,
):
    me_k = lax.axis_index("kv")
    me_t = lax.axis_index("tp")
    rows, width = wide.shape
    model = width * kv
    units = gate1.shape[0]
    pieces = -(-units // PIECE)
    ragged = units - (pieces - 1) * PIECE
    rows_t = rows // tp
    rows_k = rows // kv
    half = max(1, kv // 2)
    heads = state.shape[1]
    hd = state.shape[2]
    qw = heads * hd

    loads = []
    order = [
        (gate1_hbm, gate1), (up1_hbm, up1), (down1_hbm, down1), (wq_hbm, wq), (wk_hbm, wk),
        (wv_hbm, wv), (wg_hbm, wg), (state_hbm, state), (wo_hbm, wo),
        (gate2_hbm, gate2), (up2_hbm, up2), (down2_hbm, down2),
    ]
    for n, (src, dst) in enumerate(order):
        copy = pltpu.make_async_copy(src, dst, load_sem.at[n])
        copy.start()
        loads.append(copy)

    barrier = pltpu.get_barrier_semaphore()
    for j in range(1, kv):
        pl.semaphore_signal(barrier, 1, device_id={"kv": lax.rem(me_k + j, kv)}, device_id_type=MESH)
    for j in range(1, tp):
        pl.semaphore_signal(barrier, 1, device_id={"tp": lax.rem(me_t + j, tp)}, device_id_type=MESH)
    pl.semaphore_wait(barrier, kv + tp - 2)

    pending = []

    def exchange(axis, me, n, src_of, dst, send_sem, recv_sem):
        for j in range(1, n):
            dest = lax.rem(me + j, n)
            copy = pltpu.make_async_remote_copy(
                src_ref=src_of(dest), dst_ref=dst.at[me],
                send_sem=send_sem.at[dest], recv_sem=recv_sem.at[me],
                device_id={axis: dest}, device_id_type=MESH,
            )
            copy.start()
            pending.append(copy)

        def arrive():
            for j in range(1, n):
                source = lax.rem(me + j, n)
                pltpu.make_async_remote_copy(
                    src_ref=dst.at[source], dst_ref=dst.at[source],
                    send_sem=send_sem.at[source], recv_sem=recv_sem.at[source],
                    device_id={axis: source}, device_id_type=MESH,
                ).wait_recv()

        return arrive

    def gather_stream(phase):
        slots = stream_slots.at[phase]
        return exchange(
            "tp", me_t, tp, lambda dest: slots.at[me_t], slots,
            tp_send_sem.at[phase], tp_recv_sem.at[phase],
        )

    def widen(phase, arrive, gain_ref):
        arrive()
        for t in range(tp):
            wide[t * rows_t : (t + 1) * rows_t, :] = stream_slots[phase, t].astype(F32)
        stream = wide[...]
        lhs[...] = (stream * gain_ref[...]).astype(BF16)
        return jnp.sum(stream * stream, axis=1, keepdims=True)

    def order_of(k):
        side = lax.rem(me_k // half + 1 + k // half, 2) if kv > 1 else 0
        return side * half + lax.rem(lax.rem(me_k, half) + 1 + lax.rem(k, half), half)

    def advance(phase, factor, last):
        for t in range(tp):
            part_send[phase, t] = acc[t * rows_t : (t + 1) * rows_t, :].astype(BF16)
        slots = part_recv.at[phase]
        arrive = exchange(
            "tp", me_t, tp, lambda dest: part_send.at[phase, dest], slots,
            tp_send_sem.at[3 + phase], tp_recv_sem.at[3 + phase],
        )
        total = part_send[phase, me_t].astype(F32)
        arrive()
        for j in range(1, tp):
            total = total + part_recv[phase, lax.rem(me_t + j, tp)].astype(F32)
        fresh = (stream_slots[phase, me_t].astype(F32) + factor * total).astype(BF16)
        if last:
            out_ref[...] = fresh
            return None
        stream_slots[phase + 1, me_t] = fresh
        return gather_stream(phase + 1)

    def feed_forward(block, phase, arrive, gain_ref, w_gate, w_up, w_down, waits):
        squares = widen(phase, arrive, gain_ref)
        sq_slots[block, me_k] = jnp.broadcast_to(squares, (rows, 128))
        sq = sq_slots.at[block]
        sq_arrive = exchange(
            "kv", me_k, kv, lambda dest: sq.at[me_k], sq, sq_send_sem.at[block], sq_recv_sem.at[block]
        )
        waits[0].wait()
        waits[1].wait()

        def piece_copy(dest, p):
            return pltpu.make_async_remote_copy(
                src_ref=ff_send.at[block, dest, p], dst_ref=ff_recv.at[block, me_k, p],
                send_sem=ff_send_sem.at[block, dest, p], recv_sem=ff_recv_sem.at[block, me_k, p],
                device_id={"kv": dest}, device_id_type=MESH,
            )

        def on_piece(i, _):
            dest = order_of(lax.rem(i, kv))
            p = i // kv
            g = dest * share + p

            def multiply(columns, n):
                left = lhs[...]
                for which, w in enumerate((w_gate, w_up)):
                    ff_send[block, dest, p, which, :, 0:n] = lax.dot_general(
                        left, w[columns, :], (((1,), (1,)), ((), ())), preferred_element_type=F32
                    ).astype(BF16)

            @pl.when(g < pieces - 1)
            def _():
                multiply(pl.ds(pl.multiple_of(g * PIECE, PIECE), PIECE), PIECE)

            @pl.when(g == pieces - 1)
            def _():
                if ragged < PIECE:
                    for which in range(2):
                        ff_send[block, dest, p, which] = jnp.zeros((rows, PIECE), BF16)
                multiply(slice((pieces - 1) * PIECE, units), ragged)

            @pl.when((g < pieces) & (dest != me_k))
            def _():
                piece_copy(dest, p).start()

            return 0

        lax.fori_loop(0, kv * share, on_piece, 0)
        sq_arrive()
        total = sq_slots[block, 0]
        for k in range(1, kv):
            total = total + sq_slots[block, k]
        inverse[...] = lax.rsqrt(total / model + EPS_NORM)

        def hidden_copy(dest, p):
            slot = hidden.at[block, me_k * share + p]
            return pltpu.make_async_remote_copy(
                src_ref=slot, dst_ref=slot,
                send_sem=hid_send_sem.at[block, dest, p], recv_sem=hid_recv_sem.at[block, me_k, p],
                device_id={"kv": dest}, device_id_type=MESH,
            )

        def on_shard(p, _):
            @pl.when(me_k * share + p < pieces)
            def _():
                for j in range(1, kv):
                    source = lax.rem(me_k + j, kv)
                    slot = ff_recv.at[block, source, p]
                    pltpu.make_async_remote_copy(
                        src_ref=slot, dst_ref=slot,
                        send_sem=ff_send_sem.at[block, source, p],
                        recv_sem=ff_recv_sem.at[block, source, p],
                        device_id={"kv": source}, device_id_type=MESH,
                    ).wait_recv()
                sums = []
                for which in range(2):
                    total = ff_send[block, me_k, p, which].astype(F32)
                    for j in range(1, kv):
                        total = total + ff_recv[block, lax.rem(me_k + j, kv), p, which].astype(F32)
                    sums.append(total * inverse[:, 0:1])
                hidden[block, me_k * share + p] = (silu(sums[0]) * sums[1]).astype(BF16)
                for j in range(1, kv):
                    hidden_copy(order_of(j - 1), p).start()

            return 0

        lax.fori_loop(0, share, on_shard, 0)
        acc[...] = jnp.zeros_like(acc)
        waits[2].wait()

        def on_hidden(i, _):
            source = order_of(kv - 1 - lax.rem(i, kv))
            p = i // kv
            g = source * share + p

            @pl.when((g < pieces) & (source != me_k))
            def _():
                slot = hidden.at[block, g]
                pltpu.make_async_remote_copy(
                    src_ref=slot, dst_ref=slot,
                    send_sem=hid_send_sem.at[block, source, p],
                    recv_sem=hid_recv_sem.at[block, source, p],
                    device_id={"kv": source}, device_id_type=MESH,
                ).wait_recv()

            @pl.when(g < pieces - 1)
            def _():
                depth = pl.ds(pl.multiple_of(g * PIECE, PIECE), PIECE)
                acc[...] += jnp.dot(hidden[block, g], w_down[depth, :], preferred_element_type=F32)

            @pl.when(g == pieces - 1)
            def _():
                acc[...] += jnp.dot(
                    hidden[block, pieces - 1, :, 0:ragged],
                    w_down[(pieces - 1) * PIECE : units, :],
                    preferred_element_type=F32,
                )

            return 0

        lax.fori_loop(0, kv * share, on_hidden, 0)

        def finish():
            def on_sent(i, _):
                dest = order_of(i // share)
                p = lax.rem(i, share)

                @pl.when((dest * share + p < pieces) & (dest != me_k))
                def _():
                    piece_copy(dest, p).wait_send()

                @pl.when((me_k * share + p < pieces) & (dest != me_k))
                def _():
                    hidden_copy(dest, p).wait_send()

                return 0

            lax.fori_loop(0, kv * share, on_sent, 0)

        return finish

    stream_slots[0, me_t] = stream_ref[...]
    arrive = gather_stream(0)
    finish1 = feed_forward(0, 0, arrive, gain1_ref, gate1, up1, down1, loads[0:3])
    arrive = advance(0, 0.5, False)

    squares = widen(1, arrive, gain_mix_ref)
    row_sq[...] = jnp.broadcast_to(squares, (rows, 128))
    for k in range(kv):
        row_sq_send[k] = row_sq[k * rows_k : (k + 1) * rows_k, :]
    row_arrive = exchange(
        "kv", me_k, kv, lambda dest: row_sq_send.at[dest], row_sq_recv, row_send_sem, row_recv_sem
    )
    arrivals = []
    for n, w in enumerate((wq, wk, wv, wg)):
        loads[3 + n].wait()
        proj[...] = jnp.dot(lhs[...], w[...], preferred_element_type=F32)
        for k in range(kv):
            proj_send[n, k] = proj[k * rows_k : (k + 1) * rows_k, :].astype(BF16)
        arrivals.append(
            exchange(
                "kv", me_k, kv, lambda dest, n=n: proj_send.at[n, dest], proj_recv.at[n],
                proj_send_sem.at[n], proj_recv_sem.at[n],
            )
        )
    loads[7].wait()
    row_arrive()
    total = row_sq_send[me_k]
    for j in range(1, kv):
        total = total + row_sq_recv[lax.rem(me_k + j, kv)]
    factor = lax.rsqrt(total / model + EPS_NORM)[:, 0:1]

    def projected(n):
        arrivals[n]()
        value = proj_send[n, me_k].astype(F32)
        for j in range(1, kv):
            value = value + proj_recv[n, lax.rem(me_k + j, kv)].astype(F32)
        return value * factor

    cosine, sine = cos_ref[...], sin_ref[...]

    def rotated(value, scale):
        parts = []
        for h in range(heads):
            x = value[:, h * hd : (h + 1) * hd]
            parts.append((x * cosine + pltpu.roll(x, hd // 2, 1) * sine) * scale)
        return parts

    queries = rotated(projected(0), 1.0)
    keys = rotated(projected(1), hd ** (-0.5))
    for h in range(heads):
        padded[h, 0:rows_k, :] = queries[h]
        key_out_ref[:, h * hd : (h + 1) * hd] = keys[h]
    for h in range(heads):
        turned = padded[h].T
        for s in range(rows_k):
            carried[h, s : s + 1, :] = jnp.sum(turned[:, s : s + 1] * state[s, h], axis=0, keepdims=True)
    values = projected(2)
    value_out_ref[...] = values
    gates = silu(projected(3))
    for h in range(heads):
        head = slice(h * hd, (h + 1) * hd)
        exponent = jnp.full((1, hd), me_t * heads + h, jnp.int32).astype(F32)
        decay = 1.0 - jnp.exp2(-5.0 - exponent)
        within = jnp.sum(queries[h] * keys[h], axis=1, keepdims=True)
        mixture = decay * carried[h, 0:rows_k, :] + within * values[:, head]
        centered = mixture - jnp.mean(mixture, axis=1, keepdims=True)
        variance = jnp.mean(centered * centered, axis=1, keepdims=True)
        normed = centered * lax.rsqrt(variance + EPS_GROUP) * head_gain_ref[:, head]
        ret_slots[me_k, :, head] = (gates[:, head] * normed).astype(BF16)
    ret_arrive = exchange(
        "kv", me_k, kv, lambda dest: ret_slots.at[me_k], ret_slots, ret_send_sem, ret_recv_sem
    )
    loads[8].wait()
    ret_arrive()
    for k in range(kv):
        mixed[k * rows_k : (k + 1) * rows_k, :] = ret_slots[k].astype(F32)
    acc[...] = jnp.dot(mixed[...].astype(BF16), wo[...], preferred_element_type=F32)
    arrive = advance(1, 1.0, False)
    finish2 = feed_forward(1, 2, arrive, gain2_ref, gate2, up2, down2, loads[9:12])
    advance(2, 0.5, True)
    finish1()
    finish2()
    for copy in pending:
        copy.wait_send()


def solution(mesh):
    kv, tp = mesh.shape["kv"], mesh.shape["tp"]

    def per_device(
        stream_in, positions, ret_state, first_gain, first_gate, first_up, first_down, mix_gain,
        w_query, w_key, w_value, w_outgate, w_out, head_gain, second_gain, second_gate, second_up,
        second_down,
    ):
        rows_t, width = stream_in.shape
        rows = rows_t * tp
        seqs, heads, hd, _ = ret_state.shape
        qw = heads * hd
        units = first_gate.shape[1]
        share = -(-(-(-units // PIECE)) // kv)
        half_dim = hd // 2
        freq = 10000.0 ** (-jnp.arange(half_dim, dtype=F32) / half_dim)
        angles = positions.astype(F32)[:, None] * freq[None, :]
        cosine, sine = jnp.cos(angles), jnp.sin(angles)
        cosine = jnp.concatenate([cosine, cosine], axis=1)
        sine = jnp.concatenate([-sine, sine], axis=1)
        weights = (
            first_gate.T, first_up.T, first_down, w_query, w_key, w_value, w_outgate, w_out,
            second_gate.T, second_up.T, second_down,
        )
        vmem = pl.BlockSpec(memory_space=pltpu.VMEM)
        anywhere = pl.BlockSpec(memory_space=pl.ANY)
        dma = pltpu.SemaphoreType.DMA
        pad_rows = -(-seqs // 16) * 16
        out, keys, values = pl.pallas_call(
            functools.partial(layer_kernel, kv, tp, share),
            out_shape=(
                jax.ShapeDtypeStruct((rows_t, width), BF16),
                jax.ShapeDtypeStruct((seqs, qw), F32),
                jax.ShapeDtypeStruct((seqs, qw), F32),
            ),
            in_specs=[vmem] * 7 + [anywhere] * 12,
            out_specs=(vmem, vmem, vmem),
            scratch_shapes=[pltpu.VMEM(w.shape, BF16) for w in weights]
            + [
                pltpu.VMEM(ret_state.shape, F32),
                pltpu.VMEM((3, tp, rows_t, width), BF16),
                pltpu.VMEM((3, tp, rows_t, width), BF16),
                pltpu.VMEM((3, tp, rows_t, width), BF16),
                pltpu.VMEM((rows, width), F32),
                pltpu.VMEM((rows, width), BF16),
                pltpu.VMEM((rows, width), F32),
                pltpu.VMEM((2, kv, rows, 128), F32),
                pltpu.VMEM((rows, 128), F32),
                pltpu.VMEM((2, kv, share, 2, rows, PIECE), BF16),
                pltpu.VMEM((2, kv, share, 2, rows, PIECE), BF16),
                pltpu.VMEM((2, kv * share, rows, PIECE), BF16),
                pltpu.VMEM((rows, qw), F32),
                pltpu.VMEM((4, kv, seqs, qw), BF16),
                pltpu.VMEM((4, kv, seqs, qw), BF16),
                pltpu.VMEM((rows, 128), F32),
                pltpu.VMEM((kv, seqs, 128), F32),
                pltpu.VMEM((kv, seqs, 128), F32),
                pltpu.VMEM((heads, pad_rows, hd), F32),
                pltpu.VMEM((heads, pad_rows, hd), F32),
                pltpu.VMEM((kv, seqs, qw), BF16),
                pltpu.VMEM((rows, qw), F32),
                dma((12,)), dma((6, tp)), dma((6, tp)), dma((2, kv)), dma((2, kv)),
                dma((2, kv, share)), dma((2, kv, share)), dma((2, kv, share)), dma((2, kv, share)),
                dma((4, kv)), dma((4, kv)), dma((kv,)), dma((kv,)), dma((kv,)), dma((kv,)),
            ],
            compiler_params=pltpu.CompilerParams(
                collective_id=0, has_side_effects=True, vmem_limit_bytes=63 * 1024 * 1024
            ),
        )(
            stream_in, cosine, sine, first_gain[None, :], mix_gain[None, :], second_gain[None, :],
            head_gain[None, :], *weights[0:8], *weights[8:11], ret_state,
        )
        head_ids = (lax.axis_index("tp") * heads + jnp.arange(heads)).astype(F32)
        decays = 1.0 - 2.0 ** (-5.0 - head_ids)
        keys = keys.reshape(seqs, heads, hd)
        values = values.reshape(seqs, heads, hd)
        new_state = (
            decays[None, :, None, None] * ret_state + keys[..., :, None] * values[..., None, :]
        )
        return out, new_state

    in_specs = (
        P(("grp", "tp"), "kv"), P(("grp", "kv")), P(("grp", "kv"), "tp", None, None), P("kv"),
        P("kv", "tp"), P("kv", "tp"), P("tp", "kv"), P("kv"), P("kv", "tp"), P("kv", "tp"),
        P("kv", "tp"), P("kv", "tp"), P("tp", "kv"), P("tp"), P("kv"), P("kv", "tp"),
        P("kv", "tp"), P("tp", "kv"),
    )
    out_specs = (P(("grp", "tp"), "kv"), P(("grp", "kv"), "tp", None, None))
    return jax.shard_map(
        per_device, mesh=mesh, in_specs=in_specs, out_specs=out_specs, check_vma=False
    )
```

```python
import functools

import jax
import jax.numpy as jnp
import numpy as np
from jax import lax
from jax.experimental import pallas as pl
from jax.experimental.pallas import tpu as pltpu
from jax.sharding import PartitionSpec as P

MESH = pl.DeviceIdType.MESH
EPS_NORM = 1e-06
EPS_GROUP = 1e-05
PIECE = 256
F32 = jnp.float32
BF16 = jnp.bfloat16


def silu(v):
    return v / (1.0 + jnp.exp(-v))


def layer_kernel(
    kv, tp, share,
    stream_ref, freq_ref, sign_ref, pos_ref, gain1_ref, gain_mix_ref, gain2_ref, head_gain_ref,
    gate1_hbm, up1_hbm, down1_hbm, wq_hbm, wk_hbm, wv_hbm, wg_hbm, wo_hbm,
    gate2_hbm, up2_hbm, down2_hbm, state_hbm,
    out_ref, key_out_ref, value_out_ref,
    gate1, up1, down1, wq, wk, wv, wg, wo, gate2, up2, down2, state,
    stream_slots, part_send, part_recv, wide, lhs, acc, sq_slots, inverse,
    ff_send, ff_recv, hidden, proj, proj_send, proj_recv, row_sq, row_sq_send, row_sq_recv,
    padded, carried, ret_slots, mixed, angles, turns,
    load_sem, tp_send_sem, tp_recv_sem, sq_send_sem, sq_recv_sem,
    ff_send_sem, ff_recv_sem, hid_send_sem, hid_recv_sem,
    proj_send_sem, proj_recv_sem, row_send_sem, row_recv_sem, ret_send_sem, ret_recv_sem,
):
    me_k = lax.axis_index("kv")
    me_t = lax.axis_index("tp")
    rows, width = wide.shape
    model = width * kv
    units = gate1.shape[0]
    pieces = -(-units // PIECE)
    ragged = units - (pieces - 1) * PIECE
    rows_t = rows // tp
    rows_k = rows // kv
    half = max(1, kv // 2)
    heads = state.shape[1]
    hd = state.shape[2]
    qw = heads * hd

    loads = []
    order = [
        (gate1_hbm, gate1), (up1_hbm, up1), (down1_hbm, down1), (wq_hbm, wq), (wk_hbm, wk),
        (wv_hbm, wv), (wg_hbm, wg), (state_hbm, state), (wo_hbm, wo),
        (gate2_hbm, gate2), (up2_hbm, up2), (down2_hbm, down2),
    ]
    for n, (src, dst) in enumerate(order):
        copy = pltpu.make_async_copy(src, dst, load_sem.at[n])
        copy.start()
        loads.append(copy)

    barrier = pltpu.get_barrier_semaphore()
    for j in range(1, kv):
        pl.semaphore_signal(barrier, 1, device_id={"kv": lax.rem(me_k + j, kv)}, device_id_type=MESH)
    for j in range(1, tp):
        pl.semaphore_signal(barrier, 1, device_id={"tp": lax.rem(me_t + j, tp)}, device_id_type=MESH)
    pl.semaphore_wait(barrier, kv + tp - 2)

    pending = []

    def exchange(axis, me, n, src_of, dst, send_sem, recv_sem):
        for j in range(1, n):
            dest = lax.rem(me + j, n)
            copy = pltpu.make_async_remote_copy(
                src_ref=src_of(dest), dst_ref=dst.at[me],
                send_sem=send_sem.at[dest], recv_sem=recv_sem.at[me],
                device_id={axis: dest}, device_id_type=MESH,
            )
            copy.start()
            pending.append(copy)

        def arrive():
            for j in range(1, n):
                source = lax.rem(me + j, n)
                pltpu.make_async_remote_copy(
                    src_ref=dst.at[source], dst_ref=dst.at[source],
                    send_sem=send_sem.at[source], recv_sem=recv_sem.at[source],
                    device_id={axis: source}, device_id_type=MESH,
                ).wait_recv()

        return arrive

    def gather_stream(phase):
        slots = stream_slots.at[phase]
        return exchange(
            "tp", me_t, tp, lambda dest: slots.at[me_t], slots,
            tp_send_sem.at[phase], tp_recv_sem.at[phase],
        )

    def widen(phase, arrive, gain_ref):
        arrive()
        for t in range(tp):
            wide[t * rows_t : (t + 1) * rows_t, :] = stream_slots[phase, t].astype(F32)
        stream = wide[...]
        lhs[...] = (stream * gain_ref[...]).astype(BF16)
        return jnp.sum(stream * stream, axis=1, keepdims=True)

    def order_of(k):
        side = lax.rem(me_k // half + 1 + k // half, 2) if kv > 1 else 0
        return side * half + lax.rem(lax.rem(me_k, half) + 1 + lax.rem(k, half), half)

    def advance(phase, factor, last):
        for t in range(tp):
            part_send[phase, t] = acc[t * rows_t : (t + 1) * rows_t, :].astype(BF16)
        slots = part_recv.at[phase]
        arrive = exchange(
            "tp", me_t, tp, lambda dest: part_send.at[phase, dest], slots,
            tp_send_sem.at[3 + phase], tp_recv_sem.at[3 + phase],
        )
        total = part_send[phase, me_t].astype(F32)
        arrive()
        for j in range(1, tp):
            total = total + part_recv[phase, lax.rem(me_t + j, tp)].astype(F32)
        fresh = (stream_slots[phase, me_t].astype(F32) + factor * total).astype(BF16)
        if last:
            out_ref[...] = fresh
            return None
        stream_slots[phase + 1, me_t] = fresh
        return gather_stream(phase + 1)

    def feed_forward(block, phase, arrive, gain_ref, w_gate, w_up, w_down, waits):
        squares = widen(phase, arrive, gain_ref)
        sq_slots[block, me_k] = jnp.broadcast_to(squares, (rows, 128))
        sq = sq_slots.at[block]
        sq_arrive = exchange(
            "kv", me_k, kv, lambda dest: sq.at[me_k], sq, sq_send_sem.at[block], sq_recv_sem.at[block]
        )
        waits[0].wait()
        waits[1].wait()

        def piece_copy(dest, p):
            return pltpu.make_async_remote_copy(
                src_ref=ff_send.at[block, dest, p], dst_ref=ff_recv.at[block, me_k, p],
                send_sem=ff_send_sem.at[block, dest, p], recv_sem=ff_recv_sem.at[block, me_k, p],
                device_id={"kv": dest}, device_id_type=MESH,
            )

        def on_piece(i, _):
            dest = order_of(lax.rem(i, kv))
            p = i // kv
            g = dest * share + p

            def multiply(columns, n):
                left = lhs[...]
                for which, w in enumerate((w_gate, w_up)):
                    ff_send[block, dest, p, which, :, 0:n] = lax.dot_general(
                        left, w[columns, :], (((1,), (1,)), ((), ())), preferred_element_type=F32
                    ).astype(BF16)

            @pl.when(g < pieces - 1)
            def _():
                multiply(pl.ds(pl.multiple_of(g * PIECE, PIECE), PIECE), PIECE)

            @pl.when(g == pieces - 1)
            def _():
                if ragged < PIECE:
                    for which in range(2):
                        ff_send[block, dest, p, which] = jnp.zeros((rows, PIECE), BF16)
                multiply(slice((pieces - 1) * PIECE, units), ragged)

            @pl.when((g < pieces) & (dest != me_k))
            def _():
                piece_copy(dest, p).start()

            return 0

        lax.fori_loop(0, kv * share, on_piece, 0)
        sq_arrive()
        total = sq_slots[block, 0]
        for k in range(1, kv):
            total = total + sq_slots[block, k]
        inverse[...] = lax.rsqrt(total / model + EPS_NORM)

        def hidden_copy(dest, p):
            slot = hidden.at[block, me_k * share + p]
            return pltpu.make_async_remote_copy(
                src_ref=slot, dst_ref=slot,
                send_sem=hid_send_sem.at[block, dest, p], recv_sem=hid_recv_sem.at[block, me_k, p],
                device_id={"kv": dest}, device_id_type=MESH,
            )

        def on_shard(p, _):
            @pl.when(me_k * share + p < pieces)
            def _():
                for j in range(1, kv):
                    source = lax.rem(me_k + j, kv)
                    slot = ff_recv.at[block, source, p]
                    pltpu.make_async_remote_copy(
                        src_ref=slot, dst_ref=slot,
                        send_sem=ff_send_sem.at[block, source, p],
                        recv_sem=ff_recv_sem.at[block, source, p],
                        device_id={"kv": source}, device_id_type=MESH,
                    ).wait_recv()
                sums = []
                for which in range(2):
                    total = ff_send[block, me_k, p, which].astype(F32)
                    for j in range(1, kv):
                        total = total + ff_recv[block, lax.rem(me_k + j, kv), p, which].astype(F32)
                    sums.append(total * inverse[:, 0:1])
                hidden[block, me_k * share + p] = (silu(sums[0]) * sums[1]).astype(BF16)
                for j in range(1, kv):
                    hidden_copy(order_of(j - 1), p).start()

            return 0

        lax.fori_loop(0, share, on_shard, 0)
        acc[...] = jnp.zeros_like(acc)
        waits[2].wait()

        def on_hidden(i, _):
            source = order_of(kv - 1 - lax.rem(i, kv))
            p = i // kv
            g = source * share + p

            @pl.when((g < pieces) & (source != me_k))
            def _():
                slot = hidden.at[block, g]
                pltpu.make_async_remote_copy(
                    src_ref=slot, dst_ref=slot,
                    send_sem=hid_send_sem.at[block, source, p],
                    recv_sem=hid_recv_sem.at[block, source, p],
                    device_id={"kv": source}, device_id_type=MESH,
                ).wait_recv()

            @pl.when(g < pieces - 1)
            def _():
                depth = pl.ds(pl.multiple_of(g * PIECE, PIECE), PIECE)
                acc[...] += jnp.dot(hidden[block, g], w_down[depth, :], preferred_element_type=F32)

            @pl.when(g == pieces - 1)
            def _():
                acc[...] += jnp.dot(
                    hidden[block, pieces - 1, :, 0:ragged],
                    w_down[(pieces - 1) * PIECE : units, :],
                    preferred_element_type=F32,
                )

            return 0

        lax.fori_loop(0, kv * share, on_hidden, 0)

        def finish():
            def on_sent(i, _):
                dest = order_of(i // share)
                p = lax.rem(i, share)

                @pl.when((dest * share + p < pieces) & (dest != me_k))
                def _():
                    piece_copy(dest, p).wait_send()

                @pl.when((me_k * share + p < pieces) & (dest != me_k))
                def _():
                    hidden_copy(dest, p).wait_send()

                return 0

            lax.fori_loop(0, kv * share, on_sent, 0)

        return finish

    stream_slots[0, me_t] = stream_ref[...]
    arrive = gather_stream(0)
    for s in range(rows_k):
        angles[s : s + 1, :] = freq_ref[...] * jnp.full((1, hd), pos_ref[s], jnp.int32).astype(F32)
    turn = angles[0:rows_k, :]
    turns[0] = jnp.cos(turn)
    turns[1] = jnp.sin(turn) * sign_ref[...]
    finish1 = feed_forward(0, 0, arrive, gain1_ref, gate1, up1, down1, loads[0:3])
    arrive = advance(0, 0.5, False)

    squares = widen(1, arrive, gain_mix_ref)
    row_sq[...] = jnp.broadcast_to(squares, (rows, 128))
    for k in range(kv):
        row_sq_send[k] = row_sq[k * rows_k : (k + 1) * rows_k, :]
    row_arrive = exchange(
        "kv", me_k, kv, lambda dest: row_sq_send.at[dest], row_sq_recv, row_send_sem, row_recv_sem
    )
    arrivals = []
    for n, w in enumerate((wq, wk, wv, wg)):
        loads[3 + n].wait()
        proj[...] = jnp.dot(lhs[...], w[...], preferred_element_type=F32)
        for k in range(kv):
            proj_send[n, k] = proj[k * rows_k : (k + 1) * rows_k, :].astype(BF16)
        arrivals.append(
            exchange(
                "kv", me_k, kv, lambda dest, n=n: proj_send.at[n, dest], proj_recv.at[n],
                proj_send_sem.at[n], proj_recv_sem.at[n],
            )
        )
    loads[7].wait()
    row_arrive()
    total = row_sq_send[me_k]
    for j in range(1, kv):
        total = total + row_sq_recv[lax.rem(me_k + j, kv)]
    factor = lax.rsqrt(total / model + EPS_NORM)[:, 0:1]

    def projected(n):
        arrivals[n]()
        value = proj_send[n, me_k].astype(F32)
        for j in range(1, kv):
            value = value + proj_recv[n, lax.rem(me_k + j, kv)].astype(F32)
        return value * factor


    cosine, sine = turns[0], turns[1]

    def rotated(value, scale):
        parts = []
        for h in range(heads):
            x = value[:, h * hd : (h + 1) * hd]
            parts.append((x * cosine + pltpu.roll(x, hd // 2, 1) * sine) * scale)
        return parts

    queries = rotated(projected(0), 1.0)
    keys = rotated(projected(1), hd ** (-0.5))
    for h in range(heads):
        padded[h, 0:rows_k, :] = queries[h]
        padded[heads + h, 0:rows_k, :] = keys[h]
        key_out_ref[h] = padded[heads + h].T
    for h in range(heads):
        turned = padded[h].T
        for s in range(rows_k):
            carried[h, s : s + 1, :] = jnp.sum(turned[:, s : s + 1] * state[s, h], axis=0, keepdims=True)
    values = projected(2)
    value_out_ref[...] = values
    gates = silu(projected(3))
    for h in range(heads):
        head = slice(h * hd, (h + 1) * hd)
        decay = decay_of(me_t * heads + h, hd)
        within = jnp.sum(queries[h] * keys[h], axis=1, keepdims=True)
        mixture = decay * carried[h, 0:rows_k, :] + within * values[:, head]
        centered = mixture - jnp.mean(mixture, axis=1, keepdims=True)
        variance = jnp.mean(centered * centered, axis=1, keepdims=True)
        normed = centered * lax.rsqrt(variance + EPS_GROUP) * head_gain_ref[:, head]
        ret_slots[me_k, :, head] = (gates[:, head] * normed).astype(BF16)
    ret_arrive = exchange(
        "kv", me_k, kv, lambda dest: ret_slots.at[me_k], ret_slots, ret_send_sem, ret_recv_sem
    )
    loads[8].wait()
    ret_arrive()
    for k in range(kv):
        mixed[k * rows_k : (k + 1) * rows_k, :] = ret_slots[k].astype(F32)
    acc[...] = jnp.dot(mixed[...].astype(BF16), wo[...], preferred_element_type=F32)
    arrive = advance(1, 1.0, False)
    finish2 = feed_forward(1, 2, arrive, gain2_ref, gate2, up2, down2, loads[9:12])
    advance(2, 0.5, True)
    finish1()
    finish2()
    for copy in pending:
        copy.wait_send()


def decay_of(head, width):
    return 1.0 - jnp.exp2(-5.0 - jnp.full((1, width), head, jnp.int32).astype(F32))


def state_kernel(heads, key_ref, value_ref, state_ref, new_ref):
    decay = decay_of(lax.axis_index("tp") * heads + pl.program_id(0), state_ref.shape[3])
    for s in range(state_ref.shape[0]):
        new_ref[s, 0] = decay * state_ref[s, 0] + key_ref[0, :, s : s + 1] * value_ref[s : s + 1, :]


def solution(mesh):
    kv, tp = mesh.shape["kv"], mesh.shape["tp"]

    def per_device(
        stream_in, positions, ret_state, first_gain, first_gate, first_up, first_down, mix_gain,
        w_query, w_key, w_value, w_outgate, w_out, head_gain, second_gain, second_gate, second_up,
        second_down,
    ):
        rows_t, width = stream_in.shape
        rows = rows_t * tp
        seqs, heads, hd, _ = ret_state.shape
        qw = heads * hd
        units = first_gate.shape[1]
        share = -(-(-(-units // PIECE)) // kv)
        half_dim = hd // 2
        freq = (10000.0 ** (-np.arange(half_dim, dtype=np.float64) / half_dim)).astype(np.float32)
        freq = np.concatenate([freq, freq])[None, :]
        sign = np.concatenate([-np.ones(half_dim), np.ones(half_dim)])[None, :].astype(np.float32)
        weights = (
            first_gate.T, first_up.T, first_down, w_query, w_key, w_value, w_outgate, w_out,
            second_gate.T, second_up.T, second_down,
        )
        vmem = pl.BlockSpec(memory_space=pltpu.VMEM)
        anywhere = pl.BlockSpec(memory_space=pl.ANY)
        dma = pltpu.SemaphoreType.DMA
        pad_rows = -(-seqs // 16) * 16
        out, keys, values = pl.pallas_call(
            functools.partial(layer_kernel, kv, tp, share),
            out_shape=(
                jax.ShapeDtypeStruct((rows_t, width), BF16),
                jax.ShapeDtypeStruct((heads, hd, pad_rows), F32),
                jax.ShapeDtypeStruct((seqs, qw), F32),
            ),
            in_specs=[vmem] * 3 + [pl.BlockSpec(memory_space=pltpu.SMEM)] + [vmem] * 4 + [anywhere] * 12,
            out_specs=(vmem, vmem, vmem),
            scratch_shapes=[pltpu.VMEM(w.shape, BF16) for w in weights]
            + [
                pltpu.VMEM(ret_state.shape, F32),
                pltpu.VMEM((3, tp, rows_t, width), BF16),
                pltpu.VMEM((3, tp, rows_t, width), BF16),
                pltpu.VMEM((3, tp, rows_t, width), BF16),
                pltpu.VMEM((rows, width), F32),
                pltpu.VMEM((rows, width), BF16),
                pltpu.VMEM((rows, width), F32),
                pltpu.VMEM((2, kv, rows, 128), F32),
                pltpu.VMEM((rows, 128), F32),
                pltpu.VMEM((2, kv, share, 2, rows, PIECE), BF16),
                pltpu.VMEM((2, kv, share, 2, rows, PIECE), BF16),
                pltpu.VMEM((2, kv * share, rows, PIECE), BF16),
                pltpu.VMEM((rows, qw), F32),
                pltpu.VMEM((4, kv, seqs, qw), BF16),
                pltpu.VMEM((4, kv, seqs, qw), BF16),
                pltpu.VMEM((rows, 128), F32),
                pltpu.VMEM((kv, seqs, 128), F32),
                pltpu.VMEM((kv, seqs, 128), F32),
                pltpu.VMEM((2 * heads, pad_rows, hd), F32),
                pltpu.VMEM((heads, pad_rows, hd), F32),
                pltpu.VMEM((kv, seqs, qw), BF16),
                pltpu.VMEM((rows, qw), F32),
                pltpu.VMEM((pad_rows, hd), F32),
                pltpu.VMEM((2, seqs, hd), F32),
                dma((12,)), dma((6, tp)), dma((6, tp)), dma((2, kv)), dma((2, kv)),
                dma((2, kv, share)), dma((2, kv, share)), dma((2, kv, share)), dma((2, kv, share)),
                dma((4, kv)), dma((4, kv)), dma((kv,)), dma((kv,)), dma((kv,)), dma((kv,)),
            ],
            compiler_params=pltpu.CompilerParams(
                collective_id=0, has_side_effects=True, vmem_limit_bytes=63 * 1024 * 1024
            ),
        )(
            stream_in, freq, sign, positions, first_gain[None, :], mix_gain[None, :], second_gain[None, :],
            head_gain[None, :], *weights[0:8], *weights[8:11], ret_state,
        )
        one = lambda h: (0, h, 0, 0)
        new_state = pl.pallas_call(
            functools.partial(state_kernel, heads),
            grid=(heads,),
            out_shape=jax.ShapeDtypeStruct(ret_state.shape, F32),
            in_specs=[
                pl.BlockSpec((1, hd, pad_rows), lambda h: (h, 0, 0)),
                pl.BlockSpec((seqs, hd), lambda h: (0, h)),
                pl.BlockSpec((seqs, 1, hd, hd), one),
            ],
            out_specs=pl.BlockSpec((seqs, 1, hd, hd), one),
            compiler_params=pltpu.CompilerParams(dimension_semantics=("arbitrary",)),
        )(keys, values, ret_state)
        return out, new_state

    in_specs = (
        P(("grp", "tp"), "kv"), P(("grp", "kv")), P(("grp", "kv"), "tp", None, None), P("kv"),
        P("kv", "tp"), P("kv", "tp"), P("tp", "kv"), P("kv"), P("kv", "tp"), P("kv", "tp"),
        P("kv", "tp"), P("kv", "tp"), P("tp", "kv"), P("tp"), P("kv"), P("kv", "tp"),
        P("kv", "tp"), P("tp", "kv"),
    )
    out_specs = (P(("grp", "tp"), "kv"), P(("grp", "kv"), "tp", None, None))
    return jax.shard_map(
        per_device, mesh=mesh, in_specs=in_specs, out_specs=out_specs, check_vma=False
    )
```
